32 devices in a mesh: sp: 16 (over z, y, x), tp: 2 (over core).
Axes of the slice: x: 2, y: 2, z: 4, core: 2. Of those that a mesh axis runs over, the one named last changes fastest.
Arguments:
- latent: bfloat16 [4096, 256], P('sp'), may hold values from -6 to 6
- rotary_key: bfloat16 [4096, 64], P('sp'), may hold values from -7 to 7
- doc_ids: int32 [4096], P('sp'), may hold values from 0 to 7, never falling along the last dimension, each value on 1 to 1024 neighbouring positions
- queries_content: bfloat16 [4096, 1024], P('sp', 'tp'), may hold values from -6 to 6
- queries_rotary: bfloat16 [4096, 512], P('sp', 'tp'), may hold values from -400 to 400
- w_key_up: bfloat16 [256, 1024], replicated, may hold values from -0.375 to 0.375
- w_value_up: bfloat16 [256, 1024], replicated, may hold values from -0.375 to 0.375
- w_out: bfloat16 [1024, 2048], P('tp'), may hold values from -1.5 to 1.5
- residual: bfloat16 [4096, 2048], P(('sp', 'tp')), may hold values from -4 to 4
- norm_gain: float32 [2048], replicated, may hold values from 0.1 to 1.9
- routes: int32 [4096, 2], P(('sp', 'tp')), may hold values from 0 to 15, all different within a row; in each aligned block of 128 rows (0 to 127, 128 to 255, ...) at most 32 rows name the same one
- route_weights: float32 [4096, 2], P(('sp', 'tp')), may hold values from 0.1 to 1
- w_gate: bfloat16 [16, 2048, 3584], P('sp', None, 'tp'), may hold values from -0.125 to 0.125
- w_up: bfloat16 [16, 2048, 3584], P('sp', None, 'tp'), may hold values from -0.125 to 0.125
- w_down: bfloat16 [16, 3584, 2048], P('sp', 'tp'), may hold values from -0.09375 to 0.09375
- out_gain: float32 [2048], replicated, may hold values from 0.1 to 1.9
Outputs:
- mixed: bfloat16 [4096, 2048], P(('sp', 'tp'))
The draws below stay inside these ranges and needn't reach their ends.
Inputs may be any that keep to these rules, and one draw needn't show every extreme that they name: `doc_ids`: document numbers never fall along positions; each document holds 1 to 1024 positions, and one holds exactly 1024. `routes`: each row names 2 different experts; among the rows of one device (aligned blocks of 128 rows) no expert is named more than 32 times, and in some blocks one expert is named exactly 32 times.
All inputs are finite; a program needn't handle non-finite values.
Results may differ from the reference program's by a relative error of at most 0.014.
Values may be sent and summed in bfloat16 or wider, within the bound.
No kernel may reach another device: no remote copies, remote signals or barrier semaphores. Data moves between devices by JAX's collectives and lax.ppermute only.
A program may use at most 128 MiB of HBM per device.

```python
import math
import jax
import jax.numpy as jnp
import numpy as np
from jax import lax

D = 2048
HEADS = 8
DK = 128
DR = 64
DV = 128
RANK = 256
FF = 3584
TOPK = 2
REACH = 4
TOK_DEV = 256
TOKENS = 4096
ROWS = 128
EXPERTS = 16
CAP = 32
DOCS = 8
DOC_MOST = 1024
N_SP = 16
N_TP = 2


def rotary_base(key):
    rotary_draw = jnp.clip(jax.random.normal(jax.random.fold_in(key, 7), (TOKENS, DR), jnp.float32), -4.5, 4.5)
    return rotary_draw


def draw_rotary_key(key, part):
    return rotary_base(key).astype(jnp.bfloat16)


def draw_queries_rotary(key, part):
    drawn = jax.random.normal(jax.random.fold_in(key, 8), (TOKENS, HEADS, DR), jnp.float32)
    return drawn.reshape(TOKENS, HEADS * DR).astype(jnp.bfloat16)


def levels(stream_key, shape, cuts, smallest, high):
    gain = 1.0
    for dim, shards_of in cuts:
        steps = jax.random.uniform(jax.random.fold_in(jax.random.fold_in(stream_key, 6), dim), (shards_of,), jnp.float32, smallest / len(cuts), high / len(cuts))
        gain = gain * jnp.repeat(jnp.exp(steps), shape[dim] // shards_of).reshape((-1,) + (1,) * (len(shape) - 1 - dim))
    return gain


def split_up(amount, total, limit, skew):
    loads = [(1 << 20) // math.isqrt(rank ** skew) + 1 for rank in range(2, amount + 1)]
    rest, holding = total - limit - (amount - 1), [1] * (amount - 1)
    while rest > 0:
        movable = [i for i in range(amount - 1) if holding[i] < limit]
        mass, budget = sum([loads[i] for i in movable]), rest
        for i in movable:
            addition = min(limit - holding[i], max(1, budget * loads[i] // mass), rest)
            holding[i] = holding[i] + addition
            rest = rest - addition
    return np.array([limit] + holding)


def uneven(own_key, amount, total, bound, lean):
    if amount == 2:
        one = jax.random.randint(own_key, (), max(1, total - bound), min(bound, total - 1) + 1)
        return jnp.stack([one, total - one])
    tallies = jnp.asarray(split_up(amount, total, bound, lean), jnp.int32)
    couples = (amount - 1) // 2
    donor, sink = tallies[1:1 + 2 * couples:2], tallies[2:2 + 2 * couples:2]
    room = jnp.minimum(donor - 1, bound - sink)
    moved = jax.random.randint(jax.random.fold_in(own_key, 1), (couples,), 0, 1 << 20) % (room + 1)
    tallies = tallies.at[1:1 + 2 * couples:2].set(donor - moved).at[2:2 + 2 * couples:2].set(sink + moved)
    return tallies[jax.random.permutation(jax.random.fold_in(own_key, 2), amount)]


def assign_block(stream_key, own, number, rows, number_of, top, most, lean):
    ranking = jax.random.permutation(stream_key, number_of)
    heavy_load, ordinary = shares(number_of, rows * top, most, lean, True), shares(number_of, rows * top, most, lean, False)
    places = jnp.arange(number_of)

    def named(tallies, turn):
        used = int((tallies > 0).sum())
        fixed = max(1, used // 4)
        shifted = fixed + (places - fixed + turn * (used - fixed)) % max(1, number_of - fixed)
        return jnp.zeros((number_of,), jnp.int32).at[ranking[jnp.where(places < fixed, places, shifted)]].set(jnp.asarray(tallies, jnp.int32))

    tallies = jnp.where(number % 4 == 0, named(heavy_load, number // 4), named(ordinary, number - number // 4 - 1))
    mixed = jax.random.permutation(jax.random.fold_in(own, 3), number_of)
    donor, receiver = mixed[0:number_of // 2 * 2:2], mixed[1:number_of // 2 * 2:2]
    room = jnp.minimum(tallies[donor] - 1, most - tallies[receiver]) // 2
    room = jnp.where((donor == ranking[0]) | (receiver == ranking[0]) | (tallies[receiver] == 0), 0, jnp.maximum(room, 0))
    shifted = jax.random.randint(jax.random.fold_in(own, 4), (number_of // 2,), 0, 1 << 20) % (room + 1)
    tallies = tallies.at[donor].add(-shifted).at[receiver].add(shifted)
    labels = jnp.searchsorted(jnp.cumsum(tallies), jnp.arange(rows * top), side="right").astype(jnp.int32)
    listing = labels.reshape(top, rows).T
    listing = listing[jax.random.permutation(jax.random.fold_in(own, 1), rows)]
    turn = jax.random.randint(jax.random.fold_in(own, 2), (rows, 1), 0, top)
    return jnp.take_along_axis(listing, (jnp.arange(top)[None, :] + turn) % top, axis=1)


def shares(count, total, most, lean, full):
    weights = [(1 << 20) // math.isqrt(standing ** lean) + 1 for standing in range(1, count + 1)]
    largest = most if full else min(most, max(-(-total // count), total * weights[0] // sum(weights)))
    least = 1 if total - largest >= count - 1 else 0
    holding, rest = [largest] + [least] * (count - 1), total - largest - least * (count - 1)
    while rest > 0:
        candidates = [i for i in range(1, count) if holding[i] < largest] or [i for i in range(1, count) if holding[i] < most]
        pool, budget = sum([weights[i] for i in candidates]), rest
        for i in candidates:
            more = min(most - holding[i], max(1, budget * weights[i] // pool), rest)
            holding[i] = holding[i] + more
            rest = rest - more
    return np.array(holding)


def normal_values(rng, shape, width, limit, shards=(), held_as=jnp.bfloat16):
    entries = jax.random.normal(rng, shape, jnp.float32) * width
    if len(shards) > 0:
        entries = levels(rng, shape, shards, -0.22, 0.18) * entries
    return jnp.clip(entries, min=-limit, max=limit).astype(held_as)


def setup_inputs(seed: int = 0) -> dict:
    keys = jax.random.split(jax.random.key(seed), 17)
    latent = normal_values(keys[0], (TOKENS, RANK), 1.0, 6.0, ((0, 16),))
    rotary_key = draw_rotary_key(jax.random.fold_in(keys[16], 71), 0)
    doc_ids = jnp.searchsorted(jnp.cumsum(uneven(keys[2], DOCS, TOKENS, DOC_MOST, 2)), jnp.arange(TOKENS), side="right").astype(jnp.int32)
    queries_content = normal_values(keys[3], (TOKENS, HEADS * DK), 1.0, 6.0, ((0, 16), (1, 2)))
    queries_rotary = draw_queries_rotary(jax.random.fold_in(keys[16], 71), 0)
    w_key_up = normal_values(keys[5], (RANK, HEADS * DK), RANK ** -0.5, 0.375)
    w_value_up = normal_values(keys[6], (RANK, HEADS * DV), RANK ** -0.5, 0.375)
    w_out = normal_values(keys[7], (HEADS * DV, D), (HEADS * DV // 64) ** -0.5, 1.5, ((0, 2),))
    residual = normal_values(keys[8], (TOKENS, D), 0.5, 4.0, ((0, 32),))
    norm_gain = jnp.clip(1.0 + 0.18 * jax.random.normal(keys[9], (D,), jnp.float32), 0.1, 1.9)
    routes_keys = jax.random.split(jax.random.fold_in(keys[10], 1), TOKENS // ROWS)
    routes_turns = jax.random.permutation(jax.random.fold_in(keys[10], 3), TOKENS // ROWS)
    routes = jax.vmap(lambda own, number: assign_block(jax.random.fold_in(keys[10], 2), own, number, ROWS, EXPERTS, TOPK, CAP, 2))(routes_keys, routes_turns).reshape((TOKENS, TOPK))
    route_weights = jnp.clip(0.1 + 0.9 * jax.random.uniform(keys[11], (TOKENS, TOPK), jnp.float32) ** levels(keys[11], (TOKENS, TOPK), ((0, 32),), -0.2, 0.2), 0.1, 1.0)
    w_gate = normal_values(keys[12], (EXPERTS, D, FF), D ** -0.5, 0.125, ((0, 16), (2, 2)))
    w_up = normal_values(keys[13], (EXPERTS, D, FF), D ** -0.5, 0.125, ((0, 16), (2, 2)))
    w_down = normal_values(keys[14], (EXPERTS, FF, D), FF ** -0.5, 0.09375, ((0, 16), (1, 2)))
    out_gain = jnp.clip(1.0 + 0.18 * jax.random.normal(keys[15], (D,), jnp.float32), 0.1, 1.9)
    return {"latent": latent, "rotary_key": rotary_key, "doc_ids": doc_ids, "queries_content": queries_content, "queries_rotary": queries_rotary, "w_key_up": w_key_up, "w_value_up": w_value_up, "w_out": w_out, "residual": residual, "norm_gain": norm_gain, "routes": routes, "route_weights": route_weights, "w_gate": w_gate, "w_up": w_up, "w_down": w_down, "out_gain": out_gain}


ROPE_THETA = 500000.0
RESIDUAL_SCALE = 2.0 ** 0.5
NORM_EPSILON = 1e-05

def rotate(values, positions):
    half_width = values.shape[-1] // 2
    frequency = ROPE_THETA ** (-2.0 * jnp.arange(half_width, dtype=jnp.float32) / values.shape[-1])
    angles = positions.astype(jnp.float32)[:, None] * frequency[None, :]
    table_shape = (values.shape[0],) + (1,) * (values.ndim - 2) + (half_width,)
    cosine = jnp.cos(angles).reshape(table_shape)
    sine_part = jnp.sin(angles).reshape(table_shape)
    widened = values.astype(jnp.float32)
    first_half = widened[..., :half_width]
    second = widened[..., half_width:]
    return jnp.concatenate([first_half * cosine - second * sine_part, second * cosine + first_half * sine_part], -1)

def layer_norm(values, gain_vec):
    centre = lax.optimization_barrier(jnp.mean(values, -1, keepdims=True))
    spread = lax.optimization_barrier(jnp.mean(jnp.square(values - centre), -1, keepdims=True))
    return (values - centre) * lax.rsqrt(spread + NORM_EPSILON) * gain_vec

def reference(latent, rotary_key, doc_ids, queries_content, queries_rotary, w_key_up, w_value_up, w_out, residual, norm_gain, routes, route_weights, w_gate, w_up, w_down, out_gain):
    positions = jnp.arange(TOKENS, dtype=jnp.int32)
    key_content = jnp.dot(latent, w_key_up, preferred_element_type=jnp.float32).astype(jnp.bfloat16)
    key_content = key_content.reshape(TOKENS, HEADS, DK)
    values = jnp.dot(latent, w_value_up, preferred_element_type=jnp.float32).astype(jnp.bfloat16)
    values = values.reshape(TOKENS, HEADS, DV)
    key_rotary = rotate(rotary_key, positions).astype(jnp.bfloat16)
    query_rotary = rotate(queries_rotary.reshape(TOKENS, HEADS, DR), positions).astype(jnp.bfloat16)
    query_content = queries_content.reshape(TOKENS, HEADS, DK)
    padding = REACH * TOK_DEV
    key_pad = jnp.concatenate([jnp.zeros((padding, HEADS, DK), jnp.bfloat16), key_content], 0)
    value_pad = jnp.concatenate([jnp.zeros((padding, HEADS, DV), jnp.bfloat16), values], 0)
    rotary_pad = jnp.concatenate([jnp.zeros((padding, DR), jnp.bfloat16), key_rotary], 0)
    doc_pad = jnp.concatenate([jnp.full((padding,), -1, jnp.int32), doc_ids.astype(jnp.int32)], 0)
    position_pad = jnp.arange(TOKENS + padding, dtype=jnp.int32) - padding
    score_scale = (DK + DR) ** (-0.5)
    window = padding + TOK_DEV

    def attend_block(block_start):
        key_window = lax.dynamic_slice_in_dim(key_pad, block_start, window, 0).astype(jnp.float32)
        value_window = lax.dynamic_slice_in_dim(value_pad, block_start, window, 0).astype(jnp.float32)
        rotary_window = lax.dynamic_slice_in_dim(rotary_pad, block_start, window, 0).astype(jnp.float32)
        doc_window = lax.dynamic_slice_in_dim(doc_pad, block_start, window, 0)
        key_position = lax.dynamic_slice_in_dim(position_pad, block_start, window, 0)
        query_block = lax.dynamic_slice_in_dim(query_content, block_start, TOK_DEV, 0).astype(jnp.float32)
        turned_block = lax.dynamic_slice_in_dim(query_rotary, block_start, TOK_DEV, 0).astype(jnp.float32)
        query_doc = lax.dynamic_slice_in_dim(doc_ids.astype(jnp.int32), block_start, TOK_DEV, 0)
        query_position = lax.dynamic_slice_in_dim(positions, block_start, TOK_DEV, 0)
        scores = jnp.einsum('phd,qhd->hpq', query_block, key_window)
        scores = (scores + jnp.einsum('phd,qd->hpq', turned_block, rotary_window)) * score_scale
        allowed = (key_position[None, :] <= query_position[:, None]) & (key_position[None, :] >= 0)
        allowed = allowed & (doc_window[None, :] == query_doc[:, None])
        scores = jnp.where(allowed[None], scores, -jnp.inf)
        row_peak = lax.optimization_barrier(jnp.max(scores, -1, keepdims=True))
        lifted = jnp.exp(scores - row_peak)
        probability = (lifted / lax.optimization_barrier(jnp.sum(lifted, -1, keepdims=True))).astype(jnp.bfloat16)
        result = jnp.einsum('hpq,qhd->phd', probability.astype(jnp.float32), value_window)
        return result.astype(jnp.bfloat16)
    starts = jnp.arange(N_SP, dtype=jnp.int32) * TOK_DEV
    attended = lax.map(attend_block, starts).reshape(TOKENS, HEADS * DV)
    head_cols = HEADS * DV // N_TP
    projected = jnp.zeros((TOKENS, D), jnp.float32)
    for group in range(N_TP):
        partial_value = jnp.dot(attended[:, group * head_cols:(group + 1) * head_cols], w_out[group * head_cols:(group + 1) * head_cols], preferred_element_type=jnp.float32)
        projected = projected + partial_value.astype(jnp.bfloat16).astype(jnp.float32)
    normed = layer_norm(RESIDUAL_SCALE * residual.astype(jnp.float32) + projected, norm_gain).astype(jnp.bfloat16)
    capacity_all = N_SP * N_TP * CAP
    half_cols = FF // N_TP
    expert_ids = jnp.arange(EXPERTS, dtype=jnp.int32)

    def add_expert(running, inputs):
        expert_id, gate_w, up_w, down_w = inputs
        chosen = routes == expert_id
        member = jnp.any(chosen, 1)
        weight = lax.optimization_barrier(jnp.sum(jnp.where(chosen, route_weights, 0.0), 1))
        token_index = jnp.nonzero(member, size=capacity_all, fill_value=0)[0].astype(jnp.int32)
        live_mask = (jnp.arange(capacity_all) < jnp.sum(member.astype(jnp.int32))).astype(jnp.float32)
        token_rows = normed[token_index]
        gate_pre = jnp.dot(token_rows, gate_w, preferred_element_type=jnp.float32)
        upward = jnp.dot(token_rows, up_w, preferred_element_type=jnp.float32)
        hidden = (jax.nn.silu(gate_pre) * upward).astype(jnp.bfloat16)
        summed = jnp.zeros((capacity_all, D), jnp.float32)
        for group in range(N_TP):
            partial_value = jnp.dot(hidden[:, group * half_cols:(group + 1) * half_cols], down_w[group * half_cols:(group + 1) * half_cols], preferred_element_type=jnp.float32)
            summed = summed + partial_value.astype(jnp.bfloat16).astype(jnp.float32)
        expert_out = summed.astype(jnp.bfloat16).astype(jnp.float32)
        contribution = expert_out * (weight[token_index] * live_mask)[:, None]
        return (running.at[token_index].add(contribution), None)
    routed_sum, _ = lax.scan(add_expert, jnp.zeros((TOKENS, D), jnp.float32), (expert_ids, w_gate, w_up, w_down))
    combined = RESIDUAL_SCALE * normed.astype(jnp.float32) + routed_sum
    return layer_norm(combined, out_gain).astype(jnp.bfloat16)
```

```python
import functools

import jax
import jax.numpy as jnp
import numpy as np
from jax import lax
from jax.experimental import pallas as pl
from jax.experimental.pallas import tpu as pltpu
from jax.sharding import PartitionSpec as P


HEADS = 8
DK = 128
DR = 64
DV = 128
TOPK = 2
REACH = 4

ROPE_THETA = 500000.0
RESIDUAL_SCALE = 2.0**0.5
NORM_EPSILON = 1e-05
LANES = 128
FAR = 2.0**24
F32 = jnp.float32
BF16 = jnp.bfloat16


def dot(a, b, dims=((1,), (0,))):
    return lax.dot_general(a, b, (dims, ((), ())), preferred_element_type=F32)


def iota(shape, axis):
    return lax.broadcasted_iota(jnp.int32, shape, axis)


def call(body, outs, args, flops, limit=12, scalars=0, hbm=(), scratch=()):
    specs = [
        pl.BlockSpec(memory_space=pltpu.SMEM)
        if k < scalars
        else pl.BlockSpec(memory_space=pl.ANY if k in hbm else pltpu.VMEM)
        for k in range(len(args))
    ]
    return pl.pallas_call(
        body,
        out_shape=outs,
        in_specs=specs,
        out_specs=jax.tree.map(lambda _: pl.BlockSpec(memory_space=pltpu.VMEM), outs),
        scratch_shapes=list(scratch),
        cost_estimate=pl.CostEstimate(flops=flops, bytes_accessed=1 << 20, transcendentals=0),
        compiler_params=pltpu.CompilerParams(vmem_limit_bytes=limit * 2**20),
    )(*args)


def far(value):
    return pltpu.with_memory_space_constraint(value, pltpu.HBM)


def shape(*dims, dtype=BF16):
    return jax.ShapeDtypeStruct(dims, dtype)


def angle_tables(tok_dev, chips):
    half = DR // 2
    frequency = ROPE_THETA ** (-2.0 * np.arange(half) / DR)
    lanes = frequency[np.arange(LANES) % half]
    near = np.arange(tok_dev)[:, None] * lanes[None, :]
    base = (np.arange(chips) * tok_dev)[:, None] * lanes[None, :]
    return [np.asarray(t, np.float32) for t in (np.cos(near), np.sin(near), np.cos(base), np.sin(base))]


def turn_tables(sp, rows, near_cos, near_sin, base_cos, base_sin):
    cb, sb = base_cos[pl.ds(sp, 1), :], base_sin[pl.ds(sp, 1), :]
    cn, sn = near_cos[rows, :], near_sin[rows, :]
    sine = sb * cn + cb * sn
    low = (iota(sine.shape, 1) % DR) < DR // 2
    return cb * cn - sb * sn, jnp.where(low, -sine, sine)


def pack_kernel(where, latent, rotary, docs, nc, ns, bc, bs, own, send):
    sp, tp = where[0], where[1]
    rows = latent.shape[0]
    cosine, sine = turn_tables(sp, slice(None), nc, ns, bc, bs)
    a, b = iota((DR, LANES), 0), iota((DR, LANES), 1)
    keep = (a == b).astype(BF16)
    swap = ((a == (b ^ (DR // 2))) & (b < DR)).astype(BF16)
    turned = dot(rotary[...], keep, ((0,), (0,))) * cosine
    turned = turned + dot(rotary[...], swap, ((0,), (0,))) * sine
    marks = (iota((LANES - DR, rows), 0) == docs[...]).astype(BF16)
    shift = (a == b - DR).astype(BF16)
    turned = turned + dot(marks, shift, ((0,), (0,)))
    width = latent.shape[1]
    own[:, :width] = latent[...]
    own[:, width:] = turned.astype(BF16)
    half = send.shape[0]
    part = pl.ds(pl.multiple_of(tp * half, half), half)
    send[...] = own[part, :]


def ready_kernel(where, content, content_far, turning, turning_far, docs, routes, nc, ns, bc, bs, queries, pick0, pick1, *, capacity):
    sp, tp = where[0], where[1]
    rows = content.shape[0]
    heads_here = HEADS // 2
    part = pl.ds(pl.multiple_of(tp * rows, rows), rows)
    cosine, sine = turn_tables(sp, part, nc, ns, bc, bs)
    a, b = iota((LANES, LANES), 0), iota((LANES, LANES), 1)
    swap = (a == (b ^ (DR // 2))).astype(BF16)
    marks = (iota((LANES - DR, rows), 0) == docs[:, part]).astype(BF16)
    a, b = iota((DR, LANES), 0), iota((DR, LANES), 1)
    same = dot(marks, (a == b - DR).astype(BF16), ((0,), (0,)))
    lane = iota((rows, LANES), 1)
    barred = (same - 1.0) * FAR
    for group, (plain, spun) in enumerate(((content, turning), (content_far, turning_far))):
        for pair in range(heads_here // 2):
            raw = spun[:, pair * LANES : (pair + 1) * LANES]
            turned = raw.astype(F32) * cosine + dot(raw, swap) * sine
            for side in range(2):
                head = group * heads_here + pair * 2 + side
                local = pair * 2 + side
                queries[:, head * 256 : head * 256 + DK] = plain[:, local * DK : (local + 1) * DK]
                value = turned if side == 0 else pltpu.roll(turned, DR, 1)
                queries[:, head * 256 + DK : head * 256 + 256] = jnp.where(
                    lane < DR, value, barred
                ).astype(BF16)
    slots = pick0.shape[1]
    spread = (iota((TOPK, LANES), 0) == iota((TOPK, LANES), 1)).astype(BF16)
    turned = dot(routes[...].astype(F32).astype(BF16), spread, ((0,), (0,))).astype(jnp.int32)
    first, second = turned[:, 0:1], turned[:, 1:2]
    member = ((first == lane) | (second == lane)).astype(BF16)
    earlier = (iota((rows, rows), 0) > iota((rows, rows), 1)).astype(BF16)
    rank = dot(earlier, member)
    slot = iota((rows, slots), 1)
    for route, pick in ((first, pick0), (second, pick1)):
        place = jnp.sum(jnp.where(route == lane, rank, 0.0), 1, keepdims=True).astype(jnp.int32)
        pick[...] = (slot == (route ^ sp) * capacity + place).astype(BF16)


def layer_norm(values, gain):
    centre = jnp.mean(values, -1, keepdims=True)
    moved = values - centre
    spread = jnp.mean(jnp.square(moved), -1, keepdims=True)
    return moved * lax.rsqrt(spread + NORM_EPSILON) * gain


def attend_kernel(where, *refs, near, pieces, capacity):
    kv_own, kv_near = refs[0], refs[1 : 1 + near]
    queries, key_up, value_up, out_mine, out_theirs, residual, gain, pick0, pick1, down = refs[
        1 + near : 11 + near
    ]
    normed, down_held = refs[11 + near : 13 + near]
    outbound = refs[13 + near : 13 + near + pieces]
    packed, keys, values, attended, summed, w_mine, w_theirs, sems = refs[13 + near + pieces :]
    tp = where[1]
    copies = [
        pltpu.make_async_copy(out_mine, w_mine, sems.at[0]),
        pltpu.make_async_copy(out_theirs, w_theirs, sems.at[1]),
        pltpu.make_async_copy(down, down_held, sems.at[2]),
    ]
    for copy in copies:
        copy.start()
    own_rows = kv_own.shape[0]
    packed[:own_rows, :] = kv_own[...]
    at = own_rows
    for ref in kv_near:
        packed[at : at + ref.shape[0], :] = ref[...]
        at += ref.shape[0]
    rank = key_up.shape[0]
    latent = packed[:, :rank]
    keys[...] = dot(latent, key_up[...]).astype(BF16)
    values[...] = dot(latent, value_up[...]).astype(BF16)
    rows = queries.shape[0]
    scale = (DK + DR) ** -0.5
    ahead = iota((rows, own_rows), 1) > iota((rows, own_rows), 0) + tp * rows

    def head_step(head, carry):
        column = lax.rem(tp * (HEADS // 2) + head, HEADS) * DK
        cols = pl.ds(pl.multiple_of(column, LANES), DK)
        query = queries[:, pl.ds(pl.multiple_of(head * 256, 256), 256)]
        key = jnp.concatenate([keys[:, cols], packed[:, rank:]], 1)
        scores = dot(query, key, ((1,), (1,)))
        scores = jnp.concatenate(
            [jnp.where(ahead, -FAR, scores[:, :own_rows]), scores[:, own_rows:]], 1
        )
        peak = jnp.max(scores, -1, keepdims=True)
        lifted = jnp.exp((scores - peak) * scale)
        total = jnp.sum(lifted, -1, keepdims=True)
        mixed = dot(lifted.astype(BF16), values[:, cols]) / total
        attended[:, pl.ds(pl.multiple_of(head * DV, LANES), DV)] = mixed.astype(BF16)
        return carry

    lax.fori_loop(0, HEADS, head_step, 0)
    half = w_mine.shape[0]
    copies[0].wait()
    summed[...] = dot(attended[:, :half], w_mine[...]).astype(BF16).astype(F32)
    copies[1].wait()
    summed[...] += dot(attended[:, half:], w_theirs[...]).astype(BF16).astype(F32)
    step = 32

    def norm_step(k, carry):
        part = pl.ds(pl.multiple_of(k * step, step), step)
        value = RESIDUAL_SCALE * residual[part, :].astype(F32) + summed[part, :]
        normed[part, :] = layer_norm(value, gain[...]).astype(BF16)
        return carry

    lax.fori_loop(0, rows // step, norm_step, 0)
    both = pick0[...] + pick1[...]
    placed = dot(both, normed[...], ((0,), (0,))).astype(BF16)
    for k, ref in enumerate(outbound):
        ref[...] = placed[k * capacity : (k + 1) * capacity]
    copies[2].wait()


def expert_kernel(own, other, w_gate, w_up, w_down, mine, theirs, rows_in, hidden, *, tile):
    half = own.shape[0]
    rows_in[:half, :] = own[...]
    rows_in[half:, :] = other[...]

    def hidden_step(step, carry):
        cols = pl.ds(pl.multiple_of(step * tile, tile), tile)
        value = rows_in[...]
        gate = dot(value, w_gate[0, :, cols])
        upward = dot(value, w_up[0, :, cols])
        hidden[:, cols] = (gate / (1.0 + jnp.exp(-gate)) * upward).astype(BF16)
        return carry

    lax.fori_loop(0, hidden.shape[1] // tile, hidden_step, 0)

    def down_step(step, carry):
        cols = pl.ds(pl.multiple_of(step * tile, tile), tile)
        partial = dot(hidden[...], w_down[0, :, cols]).astype(BF16)
        mine[:, cols] = partial[:half]
        theirs[:, cols] = partial[half:]
        return carry

    lax.fori_loop(0, mine.shape[1] // tile, down_step, 0)


def experts(own, other, w_gate, w_up, w_down):
    half, width = own.shape
    hidden = w_gate.shape[2]
    rows = 2 * half
    return call(
        functools.partial(expert_kernel, tile=256),
        [shape(half, width)] * 2,
        [own, other, w_gate, w_up, w_down],
        6 * rows * width * hidden,
        limit=14,
        scratch=[pltpu.VMEM((rows, width), BF16), pltpu.VMEM((rows, hidden), BF16)],
    )


def add_kernel(a, b, *outs):
    capacity = outs[0].shape[0]
    for k, ref in enumerate(outs):
        part = slice(k * capacity, (k + 1) * capacity)
        ref[...] = (a[part, :].astype(F32) + b[part, :].astype(F32)).astype(BF16)


def pick_rows(pick0, pick1, weights, refs, stacked, summed, pieces, capacity):
    for k, ref in enumerate(refs):
        stacked[k * capacity : (k + 1) * capacity, :] = ref[...]
    rows = pick0.shape[0]
    chosen = [
        jnp.concatenate([pick[:, s * capacity : (s + 1) * capacity] for s in pieces], 1)
        for pick in (pick0, pick1)
    ]
    summed[...] = dot(jnp.concatenate(chosen, 0), stacked[...])
    spread = (iota((TOPK, LANES), 0) == iota((TOPK, LANES), 1)).astype(F32)
    weight = lax.dot_general(
        weights[...],
        spread,
        (((0,), (0,)), ((), ())),
        precision=lax.Precision.HIGHEST,
        preferred_element_type=F32,
    )
    return weight[:, 0:1], weight[:, 1:2], rows


def early_kernel(normed, pick0, pick1, weights, *refs, pieces, capacity):
    out, stacked, summed = refs[-3:]
    first, second, rows = pick_rows(pick0, pick1, weights, refs[:-3], stacked, summed, pieces, capacity)
    out[...] = RESIDUAL_SCALE * normed[...].astype(F32) + (
        summed[:rows, :] * first + summed[rows:, :] * second
    )


def final_kernel(begun, pick0, pick1, weights, gain, *refs, pieces, capacity):
    out, stacked, summed = refs[-3:]
    first, second, rows = pick_rows(pick0, pick1, weights, refs[:-3], stacked, summed, pieces, capacity)
    step = 32
    for k in range(rows // step):
        part, lower = slice(k * step, (k + 1) * step), slice(rows + k * step, rows + (k + 1) * step)
        value = begun[part, :] + (summed[part, :] * first[part] + summed[lower, :] * second[part])
        out[part, :] = layer_norm(value, gain[...]).astype(BF16)


def group_order(chips):
    order = np.arange(chips).reshape(4, chips // 4)
    half = chips // 8
    groups = [order[2:, :half], order[2:, half:], order[1], order[0]]
    return [[int(s) for s in group.reshape(-1)] for group in groups]


def per_device(
    latent,
    rotary_key,
    doc_ids,
    queries_content,
    queries_rotary,
    w_key_up,
    w_value_up,
    w_out,
    residual,
    norm_gain,
    routes,
    route_weights,
    w_gate,
    w_up,
    w_down,
    out_gain,
):
    tok_dev = latent.shape[0]
    chips = lax.axis_size("sp")
    rows, width = residual.shape
    capacity = max(2, 2 * rows * TOPK // chips)
    sp, tp = lax.axis_index("sp"), lax.axis_index("tp")
    where = jnp.stack([sp, tp]).astype(jnp.int32)
    tables = angle_tables(tok_dev, chips)
    docs = doc_ids.reshape(1, tok_dev)

    def across(value):
        return lax.ppermute(value, "tp", [(0, 1), (1, 0)])

    def exchange(value, s):
        if s == 0:
            return value
        return lax.ppermute(value, "sp", [(j, j ^ s) for j in range(chips)])

    packed_width = latent.shape[1] + LANES
    kv_own, kv_send = call(
        pack_kernel,
        [shape(tok_dev, packed_width), shape(rows, packed_width)],
        [where, far(latent), far(rotary_key.T), far(docs), *map(far, tables)],
        1 << 26,
        scalars=1,
    )
    kv_near = [
        lax.ppermute(kv_send, "sp", [(j, (j + d) % chips) for j in range(chips)])
        for d in range(REACH, 0, -1)
    ]
    out_theirs = across(w_out)
    queries_content, queries_rotary, _ = lax.optimization_barrier(
        (queries_content, queries_rotary, kv_send)
    )

    def split(value):
        mine = lax.dynamic_slice_in_dim(value, tp * rows, rows, 0)
        return mine, across(lax.dynamic_slice_in_dim(value, (1 - tp) * rows, rows, 0))

    queries_ready, pick0, pick1 = call(
        functools.partial(ready_kernel, capacity=capacity),
        [shape(rows, HEADS * 256), shape(rows, chips * capacity), shape(rows, chips * capacity)],
        [where, *split(queries_content), *split(queries_rotary), far(docs), far(routes.T), *map(far, tables)],
        1 << 26,
        scalars=1,
    )
    kv_near, queries_ready = lax.optimization_barrier((kv_near, queries_ready))
    kv_all = [jnp.concatenate(kv_near, 0)]
    kv_all.append(across(kv_all[0]))
    reach = tok_dev + sum(value.shape[0] for value in kv_all)
    args = [where, kv_own, *kv_all, queries_ready, far(w_key_up), far(w_value_up), far(w_out), out_theirs]
    hbm = (len(args) - 2, len(args) - 1, len(args) + 4)
    args += [far(residual), far(norm_gain.reshape(1, width)), pick0, pick1, far(w_down)]
    normed, w_down, *outbound = call(
        functools.partial(attend_kernel, near=len(kv_all), pieces=chips, capacity=capacity),
        [shape(rows, width), shape(*w_down.shape)] + [shape(capacity, width)] * chips,
        args,
        1 << 32,
        limit=34,
        scalars=1,
        hbm=hbm,
        scratch=[
            pltpu.VMEM((reach, packed_width), BF16),
            pltpu.VMEM((reach, HEADS * DK), BF16),
            pltpu.VMEM((reach, HEADS * DV), BF16),
            pltpu.VMEM((rows, HEADS * DV), BF16),
            pltpu.VMEM((rows, width), F32),
            pltpu.VMEM(w_out.shape, BF16),
            pltpu.VMEM(w_out.shape, BF16),
            pltpu.SemaphoreType.DMA((3,)),
        ],
    )
    groups = group_order(chips)
    w_gate, w_up, w_down = (
        pltpu.with_memory_space_constraint(w, pltpu.VMEM) for w in (w_gate, w_up, w_down)
    )
    landed, returned, done = {}, {}, {}
    for number in (0, 2, 3, 1):
        for s in groups[number]:
            landed[s] = exchange(outbound[s], s)
    after = ()
    for number in (0, 2, 1, 3):
        group = groups[number]
        own = jnp.concatenate([landed[s] for s in group], 0)
        other = across(own)
        own, other, _ = lax.optimization_barrier((own, other, after))
        mine, theirs = experts(own, other, w_gate, w_up, w_down)
        after = (mine, done.get(0, ()), done.get(1, ()))
        done[number] = call(
            add_kernel, [shape(capacity, width)] * len(group), [mine, across(theirs)], 1 << 20
        )
        for s, value in zip(group, done[number]):
            returned[s] = exchange(value, s)
    early, late = groups[0] + groups[2] + groups[3], groups[1]

    def gathered(total, pieces, body, out, extra=()):
        return call(
            functools.partial(body, pieces=pieces, capacity=capacity),
            out,
            [total, pick0, pick1, route_weights.T, *extra, *[returned[s] for s in pieces]],
            4 * rows * len(pieces) * capacity * width,
            limit=16,
            scratch=[
                pltpu.VMEM((len(pieces) * capacity, width), BF16),
                pltpu.VMEM((TOPK * rows, width), F32),
            ],
        )

    begun = gathered(normed, early, early_kernel, shape(rows, width, dtype=F32))
    return gathered(begun, late, final_kernel, shape(rows, width), [out_gain.reshape(1, width)])


def solution(mesh):
    return jax.shard_map(
        per_device,
        mesh=mesh,
        in_specs=(
            P("sp", None),
            P("sp", None),
            P("sp"),
            P("sp", "tp"),
            P("sp", "tp"),
            P(),
            P(),
            P("tp", None),
            P(("sp", "tp"), None),
            P(),
            P(("sp", "tp"), None),
            P(("sp", "tp"), None),
            P("sp", None, "tp"),
            P("sp", None, "tp"),
            P("sp", "tp", None),
            P(),
        ),
        out_specs=P(("sp", "tp"), None),
        check_vma=False,
    )
```

```python
import functools

import jax
import jax.numpy as jnp
import numpy as np
from jax import lax
from jax.experimental import pallas as pl
from jax.experimental.pallas import tpu as pltpu
from jax.sharding import PartitionSpec as P


HEADS = 8
DK = 128
DR = 64
DV = 128
TOPK = 2
REACH = 4

ROPE_THETA = 500000.0
RESIDUAL_SCALE = 2.0**0.5
NORM_EPSILON = 1e-05
LANES = 128
FAR = 2.0**24
F32 = jnp.float32
BF16 = jnp.bfloat16


def dot(a, b, dims=((1,), (0,))):
    return lax.dot_general(a, b, (dims, ((), ())), preferred_element_type=F32)


def iota(shape, axis):
    return lax.broadcasted_iota(jnp.int32, shape, axis)


def call(body, outs, args, flops, limit=12, scalars=0, hbm=(), scratch=(), after=()):
    specs = [
        pl.BlockSpec(memory_space=pltpu.SMEM)
        if k < scalars
        else pl.BlockSpec(memory_space=pl.ANY if k in hbm else pltpu.VMEM)
        for k in range(len(args))
    ]
    count = len(args)
    args = [*args, *after]
    specs += [pl.BlockSpec(memory_space=pl.ANY)] * len(after)

    def ordered(*refs):
        body(*refs[:count], *refs[len(args) :])

    return pl.pallas_call(
        ordered,
        out_shape=outs,
        in_specs=specs,
        out_specs=jax.tree.map(lambda _: pl.BlockSpec(memory_space=pltpu.VMEM), outs),
        scratch_shapes=list(scratch),
        cost_estimate=pl.CostEstimate(flops=flops, bytes_accessed=1 << 20, transcendentals=0),
        compiler_params=pltpu.CompilerParams(vmem_limit_bytes=limit * 2**20),
    )(*args)


def far(value):
    return pltpu.with_memory_space_constraint(value, pltpu.HBM)


def shape(*dims, dtype=BF16):
    return jax.ShapeDtypeStruct(dims, dtype)


def angle_tables(tok_dev, chips):
    half = DR // 2
    frequency = ROPE_THETA ** (-2.0 * np.arange(half) / DR)
    lanes = frequency[np.arange(LANES) % half]
    near = np.arange(tok_dev)[:, None] * lanes[None, :]
    base = (np.arange(chips) * tok_dev)[:, None] * lanes[None, :]
    return [np.asarray(t, np.float32) for t in (np.cos(near), np.sin(near), np.cos(base), np.sin(base))]


def turn_tables(sp, rows, near_cos, near_sin, base_cos, base_sin):
    cb, sb = base_cos[pl.ds(sp, 1), :], base_sin[pl.ds(sp, 1), :]
    cn, sn = near_cos[rows, :], near_sin[rows, :]
    sine = sb * cn + cb * sn
    low = (iota(sine.shape, 1) % DR) < DR // 2
    return cb * cn - sb * sn, jnp.where(low, -sine, sine)


def pack_kernel(where, latent, rotary, docs, nc, ns, bc, bs, own, send):
    sp, tp = where[0], where[1]
    rows = latent.shape[0]
    cosine, sine = turn_tables(sp, slice(None), nc, ns, bc, bs)
    a, b = iota((DR, LANES), 0), iota((DR, LANES), 1)
    keep = (a == b).astype(BF16)
    swap = ((a == (b ^ (DR // 2))) & (b < DR)).astype(BF16)
    turned = dot(rotary[...], keep, ((0,), (0,))) * cosine
    turned = turned + dot(rotary[...], swap, ((0,), (0,))) * sine
    marks = (iota((LANES - DR, rows), 0) == docs[...]).astype(BF16)
    shift = (a == b - DR).astype(BF16)
    turned = turned + dot(marks, shift, ((0,), (0,)))
    width = latent.shape[1]
    own[:, :width] = latent[...]
    own[:, width:] = turned.astype(BF16)
    half = send.shape[0]
    part = pl.ds(pl.multiple_of(tp * half, half), half)
    send[...] = own[part, :]


def ready_kernel(where, content, content_far, turning, turning_far, docs, routes, nc, ns, bc, bs, down, queries, pick0, pick1, down_held, sem, *, capacity):
    copy = pltpu.make_async_copy(down, down_held, sem)
    copy.start()
    sp, tp = where[0], where[1]
    rows = content.shape[0]
    heads_here = HEADS // 2
    part = pl.ds(pl.multiple_of(tp * rows, rows), rows)
    cosine, sine = turn_tables(sp, part, nc, ns, bc, bs)
    a, b = iota((LANES, LANES), 0), iota((LANES, LANES), 1)
    swap = (a == (b ^ (DR // 2))).astype(BF16)
    marks = (iota((LANES - DR, rows), 0) == docs[:, part]).astype(BF16)
    a, b = iota((DR, LANES), 0), iota((DR, LANES), 1)
    same = dot(marks, (a == b - DR).astype(BF16), ((0,), (0,)))
    lane = iota((rows, LANES), 1)
    barred = (same - 1.0) * FAR
    for group, (plain, spun) in enumerate(((content, turning), (content_far, turning_far))):
        for pair in range(heads_here // 2):
            raw = spun[:, pair * LANES : (pair + 1) * LANES]
            turned = raw.astype(F32) * cosine + dot(raw, swap) * sine
            for side in range(2):
                head = group * heads_here + pair * 2 + side
                local = pair * 2 + side
                queries[:, head * 256 : head * 256 + DK] = plain[:, local * DK : (local + 1) * DK]
                value = turned if side == 0 else pltpu.roll(turned, DR, 1)
                queries[:, head * 256 + DK : head * 256 + 256] = jnp.where(
                    lane < DR, value, barred
                ).astype(BF16)
    slots = pick0.shape[1]
    spread = (iota((TOPK, LANES), 0) == iota((TOPK, LANES), 1)).astype(BF16)
    turned = dot(routes[...].astype(F32).astype(BF16), spread, ((0,), (0,))).astype(jnp.int32)
    first, second = turned[:, 0:1], turned[:, 1:2]
    member = ((first == lane) | (second == lane)).astype(BF16)
    earlier = (iota((rows, rows), 0) > iota((rows, rows), 1)).astype(BF16)
    rank = dot(earlier, member)
    slot = iota((rows, slots), 1)
    for route, pick in ((first, pick0), (second, pick1)):
        place = jnp.sum(jnp.where(route == lane, rank, 0.0), 1, keepdims=True).astype(jnp.int32)
        pick[...] = (slot == (route ^ sp) * capacity + place).astype(BF16)
    copy.wait()


def layer_norm(values, gain):
    centre = jnp.mean(values, -1, keepdims=True)
    moved = values - centre
    spread = jnp.mean(jnp.square(moved), -1, keepdims=True)
    return moved * lax.rsqrt(spread + NORM_EPSILON) * gain


def attend_kernel(where, *refs, near, pieces, capacity):
    kv_own, kv_near = refs[0], refs[1 : 1 + near]
    queries, key_up, value_up, out_mine, out_theirs, residual, gain, pick0, pick1, gate, up = refs[
        1 + near : 12 + near
    ]
    normed, gate_held, up_held = refs[12 + near : 15 + near]
    outbound = refs[15 + near : 15 + near + pieces]
    packed, keys, values, attended, summed, w_mine, w_theirs, sems = refs[15 + near + pieces :]
    tp = where[1]
    copies = [
        pltpu.make_async_copy(out_mine, w_mine, sems.at[0]),
        pltpu.make_async_copy(out_theirs, w_theirs, sems.at[1]),
        pltpu.make_async_copy(gate, gate_held, sems.at[2]),
        pltpu.make_async_copy(up, up_held, sems.at[3]),
    ]
    for copy in copies:
        copy.start()
    own_rows = kv_own.shape[0]
    packed[:own_rows, :] = kv_own[...]
    at = own_rows
    for ref in kv_near:
        packed[at : at + ref.shape[0], :] = ref[...]
        at += ref.shape[0]
    rank = key_up.shape[0]
    latent = packed[:, :rank]
    keys[...] = dot(latent, key_up[...]).astype(BF16)
    values[...] = dot(latent, value_up[...]).astype(BF16)
    rows = queries.shape[0]
    scale = (DK + DR) ** -0.5
    ahead = iota((rows, own_rows), 1) > iota((rows, own_rows), 0) + tp * rows

    def head_step(head, carry):
        column = lax.rem(tp * (HEADS // 2) + head, HEADS) * DK
        cols = pl.ds(pl.multiple_of(column, LANES), DK)
        query = queries[:, pl.ds(pl.multiple_of(head * 256, 256), 256)]
        key = jnp.concatenate([keys[:, cols], packed[:, rank:]], 1)
        scores = dot(query, key, ((1,), (1,)))
        scores = jnp.concatenate(
            [jnp.where(ahead, -FAR, scores[:, :own_rows]), scores[:, own_rows:]], 1
        )
        peak = jnp.max(scores, -1, keepdims=True)
        lifted = jnp.exp((scores - peak) * scale)
        total = jnp.sum(lifted, -1, keepdims=True)
        mixed = dot(lifted.astype(BF16), values[:, cols]) / total
        attended[:, pl.ds(pl.multiple_of(head * DV, LANES), DV)] = mixed.astype(BF16)
        return carry

    lax.fori_loop(0, HEADS, head_step, 0, unroll=True)
    half = w_mine.shape[0]
    copies[0].wait()
    summed[...] = dot(attended[:, :half], w_mine[...]).astype(BF16).astype(F32)
    copies[1].wait()
    summed[...] += dot(attended[:, half:], w_theirs[...]).astype(BF16).astype(F32)
    step = 32

    def norm_step(k, carry):
        part = pl.ds(pl.multiple_of(k * step, step), step)
        value = RESIDUAL_SCALE * residual[part, :].astype(F32) + summed[part, :]
        normed[part, :] = layer_norm(value, gain[...]).astype(BF16)
        return carry

    lax.fori_loop(0, rows // step, norm_step, 0)
    both = pick0[...] + pick1[...]
    placed = dot(both, normed[...], ((0,), (0,))).astype(BF16)
    for k, ref in enumerate(outbound):
        ref[...] = placed[k * capacity : (k + 1) * capacity]
    copies[2].wait()
    copies[3].wait()


def expert_kernel(own, other, w_gate, w_up, w_down, mine, theirs):
    half = own.shape[0]
    value = jnp.concatenate([own[...], other[...]], 0)
    gate = dot(value, w_gate[0])
    upward = dot(value, w_up[0])
    hidden = (gate / (1.0 + jnp.exp(-gate)) * upward).astype(BF16)
    partial = dot(hidden, w_down[0]).astype(BF16)
    mine[...] = partial[:half]
    theirs[...] = partial[half:]


def experts(own, other, w_gate, w_up, w_down, after):
    half, width = own.shape
    hidden = w_gate.shape[2]
    rows = 2 * half
    return call(
        expert_kernel,
        [shape(half, width)] * 2,
        [own, other, w_gate, w_up, w_down],
        6 * rows * width * hidden,
        limit=18,
        after=after,
    )


def mark_kernel(value, out):
    out[...] = value[...]


def add_kernel(a, b, *outs):
    capacity = outs[0].shape[0]
    for k, ref in enumerate(outs):
        part = slice(k * capacity, (k + 1) * capacity)
        ref[...] = (a[part, :].astype(F32) + b[part, :].astype(F32)).astype(BF16)


def pick_rows(pick0, pick1, weights, refs, stacked, summed, pieces, capacity):
    for k, ref in enumerate(refs):
        stacked[k * capacity : (k + 1) * capacity, :] = ref[...]
    rows = pick0.shape[0]
    chosen = [
        jnp.concatenate([pick[:, s * capacity : (s + 1) * capacity] for s in pieces], 1)
        for pick in (pick0, pick1)
    ]
    summed[...] = dot(jnp.concatenate(chosen, 0), stacked[...])
    spread = (iota((TOPK, LANES), 0) == iota((TOPK, LANES), 1)).astype(F32)
    weight = lax.dot_general(
        weights[...],
        spread,
        (((0,), (0,)), ((), ())),
        precision=lax.Precision.HIGHEST,
        preferred_element_type=F32,
    )
    return weight[:, 0:1], weight[:, 1:2], rows


def early_kernel(normed, pick0, pick1, weights, *refs, pieces, capacity):
    out, stacked, summed = refs[-3:]
    first, second, rows = pick_rows(pick0, pick1, weights, refs[:-3], stacked, summed, pieces, capacity)
    out[...] = RESIDUAL_SCALE * normed[...].astype(F32) + (
        summed[:rows, :] * first + summed[rows:, :] * second
    )


def final_kernel(begun, pick0, pick1, weights, gain, *refs, pieces, capacity):
    out, stacked, summed = refs[-3:]
    first, second, rows = pick_rows(pick0, pick1, weights, refs[:-3], stacked, summed, pieces, capacity)
    step = 32
    for k in range(rows // step):
        part, lower = slice(k * step, (k + 1) * step), slice(rows + k * step, rows + (k + 1) * step)
        value = begun[part, :] + (summed[part, :] * first[part] + summed[lower, :] * second[part])
        out[part, :] = layer_norm(value, gain[...]).astype(BF16)


def group_order(chips):
    order = np.arange(chips).reshape(4, chips // 4)
    half = chips // 8
    groups = [order[2:, :half], order[2:, half:], order[1], order[0]]
    return [[int(s) for s in group.reshape(-1)] for group in groups]


def per_device(
    latent,
    rotary_key,
    doc_ids,
    queries_content,
    queries_rotary,
    w_key_up,
    w_value_up,
    w_out,
    residual,
    norm_gain,
    routes,
    route_weights,
    w_gate,
    w_up,
    w_down,
    out_gain,
):
    tok_dev = latent.shape[0]
    chips = lax.axis_size("sp")
    rows, width = residual.shape
    capacity = max(2, 2 * rows * TOPK // chips)
    sp, tp = lax.axis_index("sp"), lax.axis_index("tp")
    where = jnp.stack([sp, tp]).astype(jnp.int32)
    tables = angle_tables(tok_dev, chips)
    docs = doc_ids.reshape(1, tok_dev)

    def across(value):
        return lax.ppermute(value, "tp", [(0, 1), (1, 0)])

    def exchange(value, s):
        if s == 0:
            return value
        return lax.ppermute(value, "sp", [(j, j ^ s) for j in range(chips)])

    packed_width = latent.shape[1] + LANES
    kv_own, kv_send = call(
        pack_kernel,
        [shape(tok_dev, packed_width), shape(rows, packed_width)],
        [where, far(latent), far(rotary_key.T), far(docs), *map(far, tables)],
        1 << 26,
        scalars=1,
    )
    kv_near = [
        lax.ppermute(kv_send, "sp", [(j, (j + d) % chips) for j in range(chips)])
        for d in range(REACH, 0, -1)
    ]
    out_theirs = across(w_out)
    queries_content, queries_rotary, _ = lax.optimization_barrier(
        (queries_content, queries_rotary, kv_send)
    )

    def split(value):
        mine = lax.dynamic_slice_in_dim(value, tp * rows, rows, 0)
        return mine, across(lax.dynamic_slice_in_dim(value, (1 - tp) * rows, rows, 0))

    args = [where, *split(queries_content), *split(queries_rotary), far(docs), far(routes.T)]
    args += [*map(far, tables), far(w_down)]
    queries_ready, pick0, pick1, w_down = call(
        functools.partial(ready_kernel, capacity=capacity),
        [
            shape(rows, HEADS * 256),
            shape(rows, chips * capacity),
            shape(rows, chips * capacity),
            shape(*w_down.shape),
        ],
        args,
        1 << 26,
        scalars=1,
        hbm=(len(args) - 1,),
        scratch=[pltpu.SemaphoreType.DMA],
    )
    kv_near, queries_ready = lax.optimization_barrier((kv_near, queries_ready))
    kv_all = [jnp.concatenate(kv_near, 0)]
    kv_all.append(across(kv_all[0]))
    reach = tok_dev + sum(value.shape[0] for value in kv_all)
    args = [where, kv_own, *kv_all, queries_ready, far(w_key_up), far(w_value_up), far(w_out), out_theirs]
    hbm = (len(args) - 2, len(args) - 1, len(args) + 4, len(args) + 5)
    args += [far(residual), far(norm_gain.reshape(1, width)), pick0, pick1, far(w_gate), far(w_up)]
    normed, w_gate, w_up, *outbound = call(
        functools.partial(attend_kernel, near=len(kv_all), pieces=chips, capacity=capacity),
        [shape(rows, width), shape(*w_gate.shape), shape(*w_up.shape)] + [shape(capacity, width)] * chips,
        args,
        1 << 32,
        limit=20,
        scalars=1,
        hbm=hbm,
        scratch=[
            pltpu.VMEM((reach, packed_width), BF16),
            pltpu.VMEM((reach, HEADS * DK), BF16),
            pltpu.VMEM((reach, HEADS * DV), BF16),
            pltpu.VMEM((rows, HEADS * DV), BF16),
            pltpu.VMEM((rows, width), F32),
            pltpu.VMEM(w_out.shape, BF16),
            pltpu.VMEM(w_out.shape, BF16),
            pltpu.SemaphoreType.DMA((4,)),
        ],
    )
    groups = group_order(chips)
    w_gate, w_up, w_down = (
        pltpu.with_memory_space_constraint(w, pltpu.VMEM) for w in (w_gate, w_up, w_down)
    )
    landed, returned = {}, {}

    def send(number, pieces):
        for s, piece in zip(groups[number], pieces):
            landed[s] = exchange(piece, s)

    halves = {}

    def give_back(number, *after):
        group = groups[number]
        done = call(
            add_kernel, [shape(capacity, width)] * len(group), halves[number], 1 << 20, after=after
        )
        for s, value in zip(group, done):
            returned[s] = exchange(value, s)
        return done

    def mark(*after):
        return call(mark_kernel, shape(8, LANES), [pick0[:8, :LANES]], 1 << 20, after=after)

    def work(number, *after):
        own = jnp.concatenate([landed[s] for s in groups[number]], 0)
        other = across(own)
        return experts(own, other, w_gate, w_up, w_down, after)

    far_a, far_b, next_plane, plane = range(4)
    for number in (far_a, plane, next_plane, far_b):
        send(number, [outbound[s] for s in groups[number]])
    mine, theirs = work(plane, mark())
    halves[plane] = (mine, across(theirs))
    mine, theirs = work(far_a, mine)
    halves[far_a] = (mine, across(theirs))
    marked = mark(give_back(far_a)[0])
    mine, theirs = work(next_plane, marked)
    halves[next_plane] = (mine, across(theirs))
    mine, theirs = work(far_b, mine)
    halves[far_b] = (mine, across(theirs))
    last = give_back(far_b)[0]
    give_back(plane, last)
    give_back(next_plane, last)
    early, late = groups[far_a], groups[far_b] + groups[plane] + groups[next_plane]

    def gathered(total, pieces, body, out, extra=()):
        return call(
            functools.partial(body, pieces=pieces, capacity=capacity),
            out,
            [total, pick0, pick1, route_weights.T, *extra, *[returned[s] for s in pieces]],
            4 * rows * len(pieces) * capacity * width,
            limit=16,
            scratch=[
                pltpu.VMEM((len(pieces) * capacity, width), BF16),
                pltpu.VMEM((TOPK * rows, width), F32),
            ],
        )

    begun = gathered(normed, early, early_kernel, shape(rows, width, dtype=F32))
    return gathered(begun, late, final_kernel, shape(rows, width), [out_gain.reshape(1, width)])


def solution(mesh):
    return jax.shard_map(
        per_device,
        mesh=mesh,
        in_specs=(
            P("sp", None),
            P("sp", None),
            P("sp"),
            P("sp", "tp"),
            P("sp", "tp"),
            P(),
            P(),
            P("tp", None),
            P(("sp", "tp"), None),
            P(),
            P(("sp", "tp"), None),
            P(("sp", "tp"), None),
            P("sp", None, "tp"),
            P("sp", None, "tp"),
            P("sp", "tp", None),
            P(),
        ),
        out_specs=P(("sp", "tp"), None),
        check_vma=False,
    )
```

```python
import functools

import jax
import jax.numpy as jnp
import numpy as np
from jax import lax
from jax.experimental import pallas as pl
from jax.experimental.pallas import tpu as pltpu
from jax.sharding import PartitionSpec as P


HEADS = 8
DK = 128
DR = 64
DV = 128
TOPK = 2
REACH = 4

ROPE_THETA = 500000.0
RESIDUAL_SCALE = 2.0**0.5
NORM_EPSILON = 1e-05
LANES = 128
CARRIED = 5
FAR = 2.0**24
F32 = jnp.float32
BF16 = jnp.bfloat16


def dot(a, b, dims=((1,), (0,))):
    return lax.dot_general(a, b, (dims, ((), ())), preferred_element_type=F32)


def iota(shape, axis):
    return lax.broadcasted_iota(jnp.int32, shape, axis)


def call(body, outs, args, flops, limit=12, scalars=0, hbm=(), scratch=(), after=()):
    specs = [
        pl.BlockSpec(memory_space=pltpu.SMEM)
        if k < scalars
        else pl.BlockSpec(memory_space=pl.ANY if k in hbm else pltpu.VMEM)
        for k in range(len(args))
    ]
    count = len(args)
    args = [*args, *after]
    specs += [pl.BlockSpec(memory_space=pl.ANY)] * len(after)

    def ordered(*refs):
        body(*refs[:count], *refs[len(args) :])

    return pl.pallas_call(
        ordered,
        out_shape=outs,
        in_specs=specs,
        out_specs=jax.tree.map(lambda _: pl.BlockSpec(memory_space=pltpu.VMEM), outs),
        scratch_shapes=list(scratch),
        cost_estimate=pl.CostEstimate(flops=flops, bytes_accessed=1 << 20, transcendentals=0),
        compiler_params=pltpu.CompilerParams(vmem_limit_bytes=limit * 2**20),
    )(*args)


def far(value):
    return pltpu.with_memory_space_constraint(value, pltpu.HBM)


def shape(*dims, dtype=BF16):
    return jax.ShapeDtypeStruct(dims, dtype)


def angle_tables(tok_dev, chips):
    half = DR // 2
    frequency = ROPE_THETA ** (-2.0 * np.arange(half) / DR)
    lanes = frequency[np.arange(LANES) % half]
    near = np.arange(tok_dev)[:, None] * lanes[None, :]
    base = (np.arange(chips) * tok_dev)[:, None] * lanes[None, :]
    return [np.asarray(t, np.float32) for t in (np.cos(near), np.sin(near), np.cos(base), np.sin(base))]


def turn_tables(sp, rows, near_cos, near_sin, base_cos, base_sin):
    cb, sb = base_cos[pl.ds(sp, 1), :], base_sin[pl.ds(sp, 1), :]
    cn, sn = near_cos[rows, :], near_sin[rows, :]
    sine = sb * cn + cb * sn
    low = (iota(sine.shape, 1) % DR) < DR // 2
    return cb * cn - sb * sn, jnp.where(low, -sine, sine)


def pack_kernel(where, latent, rotary, docs, nc, ns, bc, bs, own, send):
    sp, tp = where[0], where[1]
    rows = latent.shape[0]
    cosine, sine = turn_tables(sp, slice(None), nc, ns, bc, bs)
    a, b = iota((DR, LANES), 0), iota((DR, LANES), 1)
    keep = (a == b).astype(BF16)
    swap = ((a == (b ^ (DR // 2))) & (b < DR)).astype(BF16)
    turned = dot(rotary[...], keep, ((0,), (0,))) * cosine
    turned = turned + dot(rotary[...], swap, ((0,), (0,))) * sine
    marks = (iota((LANES - DR, rows), 0) == docs[...]).astype(BF16)
    shift = (a == b - DR).astype(BF16)
    turned = turned + dot(marks, shift, ((0,), (0,)))
    width = latent.shape[1]
    own[:, :width] = latent[...]
    own[:, width:] = turned.astype(BF16)
    half = send.shape[0]
    part = pl.ds(pl.multiple_of(tp * half, half), half)
    send[...] = own[part, :]


def ready_kernel(where, content, content_far, turning, turning_far, docs, routes, nc, ns, bc, bs, *refs, capacity):
    carried, queries, pick0, pick1, held, sems = refs[:CARRIED], *refs[CARRIED : CARRIED + 3], refs[CARRIED + 3 : -1], refs[-1]
    copies = [pltpu.make_async_copy(a, b, sems.at[k]) for k, (a, b) in enumerate(zip(carried, held))]
    for copy in copies:
        copy.start()
    sp, tp = where[0], where[1]
    rows = content.shape[0]
    heads_here = HEADS // 2
    part = pl.ds(pl.multiple_of(tp * rows, rows), rows)
    cosine, sine = turn_tables(sp, part, nc, ns, bc, bs)
    a, b = iota((LANES, LANES), 0), iota((LANES, LANES), 1)
    swap = (a == (b ^ (DR // 2))).astype(BF16)
    marks = (iota((LANES - DR, rows), 0) == docs[:, part]).astype(BF16)
    a, b = iota((DR, LANES), 0), iota((DR, LANES), 1)
    same = dot(marks, (a == b - DR).astype(BF16), ((0,), (0,)))
    lane = iota((rows, LANES), 1)
    barred = (same - 1.0) * FAR
    for group, (plain, spun) in enumerate(((content, turning), (content_far, turning_far))):
        for pair in range(heads_here // 2):
            raw = spun[:, pair * LANES : (pair + 1) * LANES]
            turned = raw.astype(F32) * cosine + dot(raw, swap) * sine
            for side in range(2):
                head = group * heads_here + pair * 2 + side
                local = pair * 2 + side
                queries[:, head * 256 : head * 256 + DK] = plain[:, local * DK : (local + 1) * DK]
                value = turned if side == 0 else pltpu.roll(turned, DR, 1)
                queries[:, head * 256 + DK : head * 256 + 256] = jnp.where(
                    lane < DR, value, barred
                ).astype(BF16)
    slots = pick0.shape[1]
    spread = (iota((TOPK, LANES), 0) == iota((TOPK, LANES), 1)).astype(BF16)
    turned = dot(routes[...].astype(F32).astype(BF16), spread, ((0,), (0,))).astype(jnp.int32)
    first, second = turned[:, 0:1], turned[:, 1:2]
    member = ((first == lane) | (second == lane)).astype(BF16)
    earlier = (iota((rows, rows), 0) > iota((rows, rows), 1)).astype(BF16)
    rank = dot(earlier, member)
    slot = iota((rows, slots), 1)
    for route, pick in ((first, pick0), (second, pick1)):
        place = jnp.sum(jnp.where(route == lane, rank, 0.0), 1, keepdims=True).astype(jnp.int32)
        pick[...] = (slot == (route ^ sp) * capacity + place).astype(BF16)
    for copy in copies:
        copy.wait()


def layer_norm(values, gain):
    centre = jnp.mean(values, -1, keepdims=True)
    moved = values - centre
    spread = jnp.mean(jnp.square(moved), -1, keepdims=True)
    return moved * lax.rsqrt(spread + NORM_EPSILON) * gain


def attend_kernel(where, *refs, near, pieces, capacity):
    kv_own, kv_near = refs[0], refs[1 : 1 + near]
    queries, key_up, value_up, out_mine, out_theirs, residual, gain, pick0, pick1, gate, up = refs[
        1 + near : 12 + near
    ]
    normed, gate_held, up_held = refs[12 + near : 15 + near]
    outbound = refs[15 + near : 15 + near + pieces]
    packed, keys, values, attended, summed, w_mine, sems = refs[15 + near + pieces :]
    tp = where[1]
    copies = [
        pltpu.make_async_copy(out_mine, w_mine, sems.at[0]),
        pltpu.make_async_copy(gate, gate_held, sems.at[1]),
        pltpu.make_async_copy(up, up_held, sems.at[2]),
    ]
    for copy in copies:
        copy.start()
    own_rows = kv_own.shape[0]
    packed[:own_rows, :] = kv_own[...]
    at = own_rows
    for ref in kv_near:
        packed[at : at + ref.shape[0], :] = ref[...]
        at += ref.shape[0]
    rank = key_up.shape[0]
    latent = packed[:, :rank]
    keys[...] = dot(latent, key_up[...]).astype(BF16)
    values[...] = dot(latent, value_up[...]).astype(BF16)
    rows = queries.shape[0]
    scale = (DK + DR) ** -0.5
    ahead = iota((rows, own_rows), 1) > iota((rows, own_rows), 0) + tp * rows

    def head_step(head, carry):
        column = lax.rem(tp * (HEADS // 2) + head, HEADS) * DK
        cols = pl.ds(pl.multiple_of(column, LANES), DK)
        query = queries[:, pl.ds(pl.multiple_of(head * 256, 256), 256)]
        key = jnp.concatenate([keys[:, cols], packed[:, rank:]], 1)
        scores = dot(query, key, ((1,), (1,)))
        scores = jnp.concatenate(
            [jnp.where(ahead, -FAR, scores[:, :own_rows]), scores[:, own_rows:]], 1
        )
        peak = jnp.max(scores, -1, keepdims=True)
        lifted = jnp.exp((scores - peak) * scale)
        total = jnp.sum(lifted, -1, keepdims=True)
        mixed = dot(lifted.astype(BF16), values[:, cols]) / total
        attended[:, pl.ds(pl.multiple_of(head * DV, LANES), DV)] = mixed.astype(BF16)
        return carry

    lax.fori_loop(0, HEADS, head_step, 0, unroll=True)
    half = w_mine.shape[0]
    copies[0].wait()
    summed[...] = dot(attended[:, :half], w_mine[...]).astype(BF16).astype(F32)
    summed[...] += dot(attended[:, half:], out_theirs[...]).astype(BF16).astype(F32)
    step = 32

    def norm_step(k, carry):
        part = pl.ds(pl.multiple_of(k * step, step), step)
        value = RESIDUAL_SCALE * residual[part, :].astype(F32) + summed[part, :]
        normed[part, :] = layer_norm(value, gain[...]).astype(BF16)
        return carry

    lax.fori_loop(0, rows // step, norm_step, 0)
    both = pick0[...] + pick1[...]
    placed = dot(both, normed[...], ((0,), (0,))).astype(BF16)
    for k, ref in enumerate(outbound):
        ref[...] = placed[k * capacity : (k + 1) * capacity]
    copies[1].wait()
    copies[2].wait()


def expert_kernel(own, other, w_gate, w_up, w_down, mine, theirs):
    half = own.shape[0]
    value = jnp.concatenate([own[...], other[...]], 0)
    gate = dot(value, w_gate[0])
    upward = dot(value, w_up[0])
    hidden = (gate / (1.0 + jnp.exp(-gate)) * upward).astype(BF16)
    partial = dot(hidden, w_down[0]).astype(BF16)
    mine[...] = partial[:half]
    theirs[...] = partial[half:]


def experts(own, other, w_gate, w_up, w_down, after):
    half, width = own.shape
    hidden = w_gate.shape[2]
    rows = 2 * half
    return call(
        expert_kernel,
        [shape(half, width)] * 2,
        [own, other, w_gate, w_up, w_down],
        6 * rows * width * hidden,
        limit=18,
        after=after,
    )


def mark_kernel(value, out):
    out[...] = value[...]


def add_kernel(a, b, *outs):
    capacity = outs[0].shape[0]
    for k, ref in enumerate(outs):
        part = slice(k * capacity, (k + 1) * capacity)
        ref[...] = (a[part, :].astype(F32) + b[part, :].astype(F32)).astype(BF16)


def pick_rows(pick0, pick1, weights, refs, stacked, summed, pieces, capacity):
    for k, ref in enumerate(refs):
        stacked[k * capacity : (k + 1) * capacity, :] = ref[...]
    rows = pick0.shape[0]
    chosen = [
        jnp.concatenate([pick[:, s * capacity : (s + 1) * capacity] for s in pieces], 1)
        for pick in (pick0, pick1)
    ]
    summed[...] = dot(jnp.concatenate(chosen, 0), stacked[...])
    spread = (iota((TOPK, LANES), 0) == iota((TOPK, LANES), 1)).astype(F32)
    weight = lax.dot_general(
        weights[...],
        spread,
        (((0,), (0,)), ((), ())),
        precision=lax.Precision.HIGHEST,
        preferred_element_type=F32,
    )
    return weight[:, 0:1], weight[:, 1:2], rows


def early_kernel(normed, pick0, pick1, weights, *refs, pieces, capacity):
    out, stacked, summed = refs[-3:]
    first, second, rows = pick_rows(pick0, pick1, weights, refs[:-3], stacked, summed, pieces, capacity)
    out[...] = RESIDUAL_SCALE * normed[...].astype(F32) + (
        summed[:rows, :] * first + summed[rows:, :] * second
    )


def final_kernel(begun, pick0, pick1, weights, gain, *refs, pieces, capacity):
    out, stacked, summed = refs[-3:]
    first, second, rows = pick_rows(pick0, pick1, weights, refs[:-3], stacked, summed, pieces, capacity)
    step = 32
    for k in range(rows // step):
        part, lower = slice(k * step, (k + 1) * step), slice(rows + k * step, rows + (k + 1) * step)
        value = begun[part, :] + (summed[part, :] * first[part] + summed[lower, :] * second[part])
        out[part, :] = layer_norm(value, gain[...]).astype(BF16)


def group_order(chips):
    order = np.arange(chips).reshape(4, chips // 4)
    beyond = order[2:].T.reshape(-1)
    cut = chips // 4
    groups = [beyond[:cut], beyond[cut:], order[1], order[0]]
    return [[int(s) for s in group.reshape(-1)] for group in groups]


def per_device(
    latent,
    rotary_key,
    doc_ids,
    queries_content,
    queries_rotary,
    w_key_up,
    w_value_up,
    w_out,
    residual,
    norm_gain,
    routes,
    route_weights,
    w_gate,
    w_up,
    w_down,
    out_gain,
):
    tok_dev = latent.shape[0]
    chips = lax.axis_size("sp")
    rows, width = residual.shape
    capacity = max(2, 2 * rows * TOPK // chips)
    sp, tp = lax.axis_index("sp"), lax.axis_index("tp")
    where = jnp.stack([sp, tp]).astype(jnp.int32)
    tables = angle_tables(tok_dev, chips)
    docs = doc_ids.reshape(1, tok_dev)

    def across(value):
        return lax.ppermute(value, "tp", [(0, 1), (1, 0)])

    def exchange(value, s):
        if s == 0:
            return value
        return lax.ppermute(value, "sp", [(j, j ^ s) for j in range(chips)])

    packed_width = latent.shape[1] + LANES
    kv_own, kv_send = call(
        pack_kernel,
        [shape(tok_dev, packed_width), shape(rows, packed_width)],
        [where, far(latent), far(rotary_key.T), far(docs), *map(far, tables)],
        1 << 26,
        scalars=1,
    )
    kv_near = [
        lax.ppermute(kv_send, "sp", [(j, (j + d) % chips) for j in range(chips)])
        for d in range(REACH, 0, -1)
    ]
    out_theirs = across(w_out)
    queries_content, queries_rotary, _ = lax.optimization_barrier(
        (queries_content, queries_rotary, kv_send)
    )

    def split(value):
        mine = lax.dynamic_slice_in_dim(value, tp * rows, rows, 0)
        return mine, across(lax.dynamic_slice_in_dim(value, (1 - tp) * rows, rows, 0))

    args = [where, *split(queries_content), *split(queries_rotary), far(docs), far(routes.T)]
    carried = [w_key_up, w_value_up, residual, norm_gain.reshape(1, width), w_down]
    args += [*map(far, tables), *map(far, carried)]
    queries_ready, pick0, pick1, w_key_up, w_value_up, residual, norm_gain, w_down = call(
        functools.partial(ready_kernel, capacity=capacity),
        [
            shape(rows, HEADS * 256),
            shape(rows, chips * capacity),
            shape(rows, chips * capacity),
            *[shape(*value.shape, dtype=value.dtype) for value in carried],
        ],
        args,
        1 << 26,
        scalars=1,
        hbm=range(len(args) - CARRIED, len(args)),
        scratch=[pltpu.SemaphoreType.DMA((CARRIED,))],
    )
    kv_near, queries_ready = lax.optimization_barrier((kv_near, queries_ready))
    kv_all = [jnp.concatenate(kv_near, 0)]
    kv_all.append(across(kv_all[0]))
    reach = tok_dev + sum(value.shape[0] for value in kv_all)
    args = [where, kv_own, *kv_all, queries_ready, w_key_up, w_value_up, far(w_out), out_theirs]
    hbm = (len(args) - 2, len(args) + 4, len(args) + 5)
    args += [residual, norm_gain, pick0, pick1, far(w_gate), far(w_up)]
    normed, w_gate, w_up, *outbound = call(
        functools.partial(attend_kernel, near=len(kv_all), pieces=chips, capacity=capacity),
        [shape(rows, width), shape(*w_gate.shape), shape(*w_up.shape)] + [shape(capacity, width)] * chips,
        args,
        1 << 32,
        limit=18,
        scalars=1,
        hbm=hbm,
        scratch=[
            pltpu.VMEM((reach, packed_width), BF16),
            pltpu.VMEM((reach, HEADS * DK), BF16),
            pltpu.VMEM((reach, HEADS * DV), BF16),
            pltpu.VMEM((rows, HEADS * DV), BF16),
            pltpu.VMEM((rows, width), F32),
            pltpu.VMEM(w_out.shape, BF16),
            pltpu.SemaphoreType.DMA((3,)),
        ],
    )
    groups = group_order(chips)
    w_gate, w_up, w_down = (
        pltpu.with_memory_space_constraint(w, pltpu.VMEM) for w in (w_gate, w_up, w_down)
    )
    landed, returned = {}, {}

    def send(number, pieces):
        for s, piece in zip(groups[number], pieces):
            landed[s] = exchange(piece, s)

    halves = {}

    def give_back(number, *after):
        group = groups[number]
        done = call(
            add_kernel, [shape(capacity, width)] * len(group), halves[number], 1 << 20, after=after
        )
        for s, value in zip(group, done):
            returned[s] = exchange(value, s)
        return done

    def mark(*after):
        return call(mark_kernel, shape(8, LANES), [pick0[:8, :LANES]], 1 << 20, after=after)

    def work(number, *after):
        own = jnp.concatenate([landed[s] for s in groups[number]], 0)
        other = across(own)
        return experts(own, other, w_gate, w_up, w_down, after)

    far_a, far_b, next_plane, plane = range(4)
    for number in (far_a, plane, next_plane, far_b):
        send(number, [outbound[s] for s in groups[number]])
    mine, theirs = work(plane, mark())
    halves[plane] = (mine, across(theirs))
    mine, theirs = work(far_a, mine)
    halves[far_a] = (mine, across(theirs))
    marked = mark(give_back(far_a)[0])
    mine, theirs = work(next_plane, marked)
    halves[next_plane] = (mine, across(theirs))
    given = give_back(plane, mine)[0]
    mine, theirs = work(far_b, mine, given)
    halves[far_b] = (mine, across(theirs))
    last = give_back(far_b)[0]
    give_back(next_plane, last)
    early, late = groups[far_a] + groups[plane], groups[far_b] + groups[next_plane]

    def gathered(total, pieces, body, out, extra=()):
        return call(
            functools.partial(body, pieces=pieces, capacity=capacity),
            out,
            [total, pick0, pick1, route_weights.T, *extra, *[returned[s] for s in pieces]],
            4 * rows * len(pieces) * capacity * width,
            limit=16,
            scratch=[
                pltpu.VMEM((len(pieces) * capacity, width), BF16),
                pltpu.VMEM((TOPK * rows, width), F32),
            ],
        )

    begun = gathered(normed, early, early_kernel, shape(rows, width, dtype=F32))
    return gathered(begun, late, final_kernel, shape(rows, width), [out_gain.reshape(1, width)])


def solution(mesh):
    return jax.shard_map(
        per_device,
        mesh=mesh,
        in_specs=(
            P("sp", None),
            P("sp", None),
            P("sp"),
            P("sp", "tp"),
            P("sp", "tp"),
            P(),
            P(),
            P("tp", None),
            P(("sp", "tp"), None),
            P(),
            P(("sp", "tp"), None),
            P(("sp", "tp"), None),
            P("sp", None, "tp"),
            P("sp", None, "tp"),
            P("sp", "tp", None),
            P(),
        ),
        out_specs=P(("sp", "tp"), None),
        check_vma=False,
    )
```
